32 devices in a mesh: sp: 8 (over z, y), tp: 4 (over x, core).
Axes of the slice: x: 2, y: 2, z: 4, core: 2. Of those that a mesh axis runs over, the one named last changes fastest.
Arguments:
- queries: bfloat16 [4096, 1024], P('sp', 'tp'), may hold values from -6 to 6
- keys: bfloat16 [4096, 1024], P('sp', 'tp'), may hold values from -6 to 6
- values: bfloat16 [4096, 1024], P('sp', 'tp'), may hold values from -12 to 12
- breaks: bfloat16 [4096, 8], P('sp', 'tp'), may hold values from -12 to 0.5
- residual_in: bfloat16 [4096, 2048], P('sp', 'tp'), may hold values from -6 to 6
- out_weight: bfloat16 [1024, 2048], P('tp'), may hold values from -0.1875 to 0.1875
- first_gain: float32 [2048], replicated, may hold values from 0.1 to 1.9
- first_shift: float32 [2048], replicated, may hold values from -2 to 2
- up_weight: bfloat16 [2048, 8192], P('sp', 'tp'), may hold values from -0.125 to 0.125
- down_weight: bfloat16 [2048, 8192], P('sp', 'tp'), may hold values from -0.0625 to 0.0625
- second_gain: float32 [2048], replicated, may hold values from 0.1 to 1.9
- second_shift: float32 [2048], replicated, may hold values from -2 to 2
Outputs:
- layer_out: bfloat16 [4096, 2048], P('sp', 'tp')
The draws below stay inside these ranges and needn't reach their ends.
All inputs are finite; a program needn't handle non-finite values.
Results may differ from the reference program's by a relative error of at most 0.018.
Values may be sent and summed in bfloat16 or wider, within the bound.
A program may use at most 128 MiB of HBM per device.

```python
import math
import jax
import jax.numpy as jnp
from jax import lax

D = 2048
FF = 8192
HEAD_COUNT = 8
HD = 128
KEY_BLOCK = 512
TOK_DEV = 512
SEQUENCE_LENGTH = 4096
N_TP = 4


def draw_values(key, part):
    offset_key, noise_key = jax.random.split(jax.random.fold_in(key, 29), 2)
    offset = jax.random.normal(offset_key, (HEAD_COUNT * HD,), jnp.float32) * 1.5
    noise = jax.random.normal(noise_key, (SEQUENCE_LENGTH, HEAD_COUNT * HD), jnp.float32) * 2.0
    return jnp.clip(noise + offset[None, :], -12.0, 12.0).astype(jnp.bfloat16)


def draw_breaks(key, part):
    gradual_key, quick_key, key_tile_rows, noise_key, spike_key, height_key = jax.random.split(jax.random.fold_in(key, 17), 6)
    slow_share = 0.5
    slow_heads = jax.random.uniform(gradual_key, (HEAD_COUNT,)) < slow_share
    slow_base = math.log(1.0 / SEQUENCE_LENGTH) - 0.5
    fast_base = -4.2 + jax.random.uniform(quick_key, (HEAD_COUNT,), minval=-0.3, maxval=0.3)
    head_base = jnp.where(slow_heads, slow_base, fast_base)
    by_block = jax.random.uniform(key_tile_rows, (SEQUENCE_LENGTH // TOK_DEV, HEAD_COUNT), minval=0.0, maxval=math.log(2.5))
    blockwise = jnp.repeat(by_block, TOK_DEV, axis=0)
    jitter = jax.random.uniform(noise_key, (SEQUENCE_LENGTH, HEAD_COUNT), minval=-0.35, maxval=0.35)
    height_values = head_base[None, :] + blockwise + jitter
    spiky_scores = jax.random.uniform(spike_key, (SEQUENCE_LENGTH, HEAD_COUNT)) < 4.0 / SEQUENCE_LENGTH
    spike_height = jax.random.uniform(height_key, (SEQUENCE_LENGTH, HEAD_COUNT), minval=-1.5, maxval=0.0)
    return jnp.where(spiky_scores, spike_height, height_values).astype(jnp.bfloat16)


def block_scale(rng, shape, cuts, least, high):
    level = 1.0
    for dim, parts in cuts:
        heights = jax.random.uniform(jax.random.fold_in(jax.random.fold_in(rng, 6), dim), (parts,), jnp.float32, least / len(cuts), high / len(cuts))
        level = level * jnp.repeat(jnp.exp(heights), shape[dim] // parts).reshape((-1,) + (1,) * (len(shape) - 1 - dim))
    return level


def scatter_about(own_key, extent, width, limit, cuts=(), kind=jnp.bfloat16):
    factor_of = block_scale(own_key, extent, cuts, -0.22, 0.18) if cuts else 1.0
    drawn = jax.random.normal(own_key, extent, jnp.float32) * width * factor_of
    return jnp.minimum(jnp.maximum(drawn, -limit), limit).astype(kind)


def setup_inputs(seed: int = 0) -> dict:
    seeds = jax.random.split(jax.random.key(seed), 13)
    queries = scatter_about(seeds[0], (SEQUENCE_LENGTH, HEAD_COUNT * HD), 1.0, 6.0, ((0, 8), (1, 4)))
    keys = scatter_about(seeds[1], (SEQUENCE_LENGTH, HEAD_COUNT * HD), 1.0, 6.0, ((0, 8), (1, 4)))
    values = draw_values(jax.random.fold_in(seeds[12], 71), 0)
    breaks = draw_breaks(jax.random.fold_in(seeds[12], 71), 0)
    residual_in = scatter_about(seeds[4], (SEQUENCE_LENGTH, D), 1.0, 6.0, ((0, 8), (1, 4)))
    out_weight = scatter_about(seeds[5], (HEAD_COUNT * HD, D), (HEAD_COUNT * HD) ** -0.5, 0.1875, ((0, 4),))
    first_gain = jnp.clip(1.0 + 0.18 * jax.random.normal(seeds[6], (D,), jnp.float32), 0.1, 1.9)
    first_shift = scatter_about(seeds[7], (D,), 0.3, 2.0, (), jnp.float32)
    up_weight = scatter_about(seeds[8], (D, FF), D ** -0.5, 0.125, ((0, 8), (1, 4)))
    down_weight = scatter_about(seeds[9], (D, FF), FF ** -0.5, 0.0625, ((0, 8), (1, 4)))
    second_gain = jnp.clip(1.0 + 0.18 * jax.random.normal(seeds[10], (D,), jnp.float32), 0.1, 1.9)
    second_shift = scatter_about(seeds[11], (D,), 0.3, 2.0, (), jnp.float32)
    return dict(queries=queries, keys=keys, values=values, breaks=breaks, residual_in=residual_in, out_weight=out_weight, first_gain=first_gain, first_shift=first_shift, up_weight=up_weight, down_weight=down_weight, second_gain=second_gain, second_shift=second_shift)


ALPHA = 2.0 ** 0.25
EPSILON = 1e-05

def rounded(partial_value):
    return lax.optimization_barrier(partial_value.astype(jnp.bfloat16)).astype(jnp.float32)

def layer_norm(pre, gain, shift):
    center = lax.optimization_barrier(jnp.mean(pre, axis=-1, keepdims=True))
    centered = pre - center
    spread = lax.optimization_barrier(jnp.mean(centered * centered, axis=-1, keepdims=True))
    return centered * lax.rsqrt(spread + EPSILON) * gain + shift

def reference(queries, keys, values, breaks, residual_in, out_weight, first_gain, first_shift, up_weight, down_weight, second_gain, second_shift):
    query_heads = queries.reshape(SEQUENCE_LENGTH, HEAD_COUNT, HD).astype(jnp.float32)
    key_heads = keys.reshape(SEQUENCE_LENGTH, HEAD_COUNT, HD).astype(jnp.float32)
    value_heads = values.reshape(SEQUENCE_LENGTH, HEAD_COUNT, HD).astype(jnp.float32)
    break_rows = breaks.astype(jnp.float32).T
    positions = jnp.arange(SEQUENCE_LENGTH, dtype=jnp.int32)
    scale = HD ** (-0.5)

    def attend_block(index):
        first = index * KEY_BLOCK
        query_block = lax.dynamic_slice_in_dim(query_heads, first, KEY_BLOCK, 0)
        query_pos = first + jnp.arange(KEY_BLOCK, dtype=jnp.int32)
        scores = jnp.einsum('qhd,khd->hqk', query_block, key_heads) * scale + break_rows[:, None, :]
        strict = (positions[None, :] < query_pos[:, None])[None]
        log_break = jax.nn.log_sigmoid(scores)
        log_keep = jnp.where(strict, log_break - scores, 0.0)
        later = lax.cumsum(log_keep, axis=2, reverse=True) - log_keep
        weights = jnp.where(strict, jnp.exp(log_break + later), 0.0).astype(jnp.bfloat16)
        mixed_heads = jnp.einsum('hqk,khd->qhd', weights.astype(jnp.float32), value_heads)
        return mixed_heads.reshape(KEY_BLOCK, HEAD_COUNT * HD).astype(jnp.bfloat16)
    attended = lax.map(attend_block, jnp.arange(SEQUENCE_LENGTH // KEY_BLOCK, dtype=jnp.int32)).reshape(SEQUENCE_LENGTH, HEAD_COUNT * HD)
    group_width = HEAD_COUNT * HD // N_TP
    attended_groups = attended.reshape(SEQUENCE_LENGTH, N_TP, group_width).transpose(1, 0, 2)
    out_groups = out_weight.reshape(N_TP, group_width, D)

    def add_group(total, pair):
        return (total + rounded(jnp.dot(pair[0], pair[1], preferred_element_type=jnp.float32)), None)
    mixed = lax.scan(add_group, jnp.zeros((SEQUENCE_LENGTH, D), jnp.float32), (attended_groups, out_groups))[0]
    first_out = layer_norm(ALPHA * residual_in.astype(jnp.float32) + mixed, first_gain, first_shift).astype(jnp.bfloat16)
    hidden_width = FF // N_TP
    up_groups = up_weight.reshape(D, N_TP, hidden_width).transpose(1, 0, 2)
    down_groups = down_weight.reshape(D, N_TP, hidden_width).transpose(1, 0, 2)

    def add_hidden(total, pair):
        activated = jnp.square(jax.nn.relu(jnp.dot(first_out, pair[0], preferred_element_type=jnp.float32))).astype(jnp.bfloat16)
        partial_value = lax.dot_general(activated, pair[1], (((1,), (1,)), ((), ())), preferred_element_type=jnp.float32)
        return (total + rounded(partial_value), None)
    channel_mix = lax.scan(add_hidden, jnp.zeros((SEQUENCE_LENGTH, D), jnp.float32), (up_groups, down_groups))[0]
    second = layer_norm(ALPHA * first_out.astype(jnp.float32) + channel_mix, second_gain, second_shift)
    return second.astype(jnp.bfloat16)
```

```python
import functools

import jax
import jax.numpy as jnp
from jax import lax
from jax.experimental import pallas as pl
from jax.experimental.pallas import tpu as pltpu
from jax.sharding import PartitionSpec as P

ALPHA = 2.0**0.25
EPSILON = 1e-05
MESH = pl.DeviceIdType.MESH
F32 = jnp.float32
BF16 = jnp.bfloat16
KV, UP, DOWN = 0, 1, 2
RIGHT, LEFT = 0, 1


def aligned(start, size):
    return pl.ds(pl.multiple_of(start, size), size)


def layer_kernel(
    n,
    t,
    heads,
    q_ref,
    kv_in,
    br_in,
    res_in,
    ow_in,
    g1_ref,
    b1_ref,
    up_in,
    down_in,
    g2_ref,
    b2_ref,
    out_ref,
    kv,
    up,
    down,
    br,
    ow,
    res,
    later_sum,
    totals,
    att_all,
    lower,
    pre,
    first,
    activated,
    part,
    mix,
    stat,
    ring_send,
    ring_recv,
    br_send,
    br_recv,
    ow_send,
    ow_recv,
    res_send,
    res_recv,
    att_send,
    att_recv,
    mix_send,
    mix_recv,
    stat_send,
    stat_recv,
    local_sem,
):
    me = lax.axis_index("sp")
    me_t = lax.axis_index("tp")
    tok = q_ref.shape[0]
    width = q_ref.shape[1]
    hd = width // heads
    feat = first.shape[1]
    cols = feat // t
    block = feat // n
    per = n // t
    half_n = n // 2

    def at_pos(p):
        p = lax.rem(p + n, n)
        back = p // half_n
        return 2 * (p + back * (n - 1 - 2 * p)) + back

    pos = me // 2 + lax.rem(me, 2) * (n - 1 - 2 * (me // 2))
    next_dev = (at_pos(pos + 1), at_pos(pos - 1))
    own_in = (kv_in, up_in, down_in)
    full = (kv, up, down)
    rows_of = (tok, block, block)

    def ring_copy(item, way, hop, piece, own=False):
        rows = rows_of[item]
        half = rows // 2
        owner = at_pos(pos - (hop - 1) if way == RIGHT else pos + (hop - 1))
        dst = full[item].at[aligned(owner * rows + piece * half, half)]
        src = own_in[item].at[aligned(piece * half, half)] if own else dst
        return pltpu.make_async_remote_copy(
            src_ref=src,
            dst_ref=dst,
            send_sem=ring_send.at[item, way, hop, piece],
            recv_sem=ring_recv.at[item, way, hop, piece],
            device_id={"sp": next_dev[way]},
            device_id_type=MESH,
        )

    def ring_landed(item, way, hop, piece):
        rows = rows_of[item]
        half = rows // 2
        owner = at_pos(pos - hop if way == RIGHT else pos + hop)
        dst = full[item].at[aligned(owner * rows + piece * half, half)]
        return pltpu.make_async_remote_copy(
            src_ref=dst,
            dst_ref=dst,
            send_sem=ring_send.at[item, way, hop, piece],
            recv_sem=ring_recv.at[item, way, hop, piece],
            device_id={"sp": next_dev[way]},
            device_id_type=MESH,
        )

    def start_own(item):
        ring_copy(item, RIGHT, 1, 0, own=True).start()
        ring_copy(item, LEFT, 1, 1, own=True).start()
        ring_copy(item, RIGHT, 1, 1, own=True).start()
        ring_copy(item, LEFT, 1, 0, own=True).start()

    def event(item, e, hop=None, second=None):
        static = isinstance(e, int)
        hop = 1 + e // 2
        second = e % 2 if static else lax.rem(e, 2)
        ring_landed(item, RIGHT, hop, second).wait_recv()

        def forward_right():
            ring_copy(item, RIGHT, hop + 1, second).start()

        def forward_left():
            ring_copy(item, LEFT, hop + 1, 1 - second).start()

        def start_next():
            if item < DOWN:
                start_own(item + 1)

        def guarded(cond, fn):
            if static:
                if cond:
                    fn()
            else:
                pl.when(cond)(fn)

        guarded(e < n - 3, forward_right)
        ring_landed(item, LEFT, hop, 1 - second).wait_recv()
        guarded(e < n - 3, forward_left)
        guarded(e == n - 4, start_next)

    def drain_sends(item):
        def one(e, _):
            hop = 1 + e // 2
            second = lax.rem(e, 2)
            ring_copy(item, RIGHT, hop, second).wait_send()
            ring_copy(item, LEFT, hop, 1 - second).wait_send()
            return 0

        lax.fori_loop(0, n - 1, one, 0)

    def peer_t(d):
        return lax.rem(me_t + d, t)

    def tp_copy(src, dst_of, sends, recvs, d):
        return pltpu.make_async_remote_copy(
            src_ref=src,
            dst_ref=dst_of(me_t),
            send_sem=sends.at[d],
            recv_sem=recvs.at[d],
            device_id={"tp": peer_t(d)},
            device_id_type=MESH,
        )

    def tp_landed(dst_of, sends, recvs, d):
        dst = dst_of(lax.rem(me_t + t - d, t))
        return pltpu.make_async_remote_copy(
            src_ref=dst,
            dst_ref=dst,
            send_sem=sends.at[d],
            recv_sem=recvs.at[d],
            device_id={"tp": peer_t(d)},
            device_id_type=MESH,
        )

    def br_copy(d, landed=False):
        owner = lax.rem(me + n - d, n) if landed else me
        return pltpu.make_async_remote_copy(
            src_ref=br.at[owner] if landed else br_in,
            dst_ref=br.at[owner],
            send_sem=br_send.at[d],
            recv_sem=br_recv.at[d],
            device_id={"sp": lax.rem(me + d, n)},
            device_id_type=MESH,
        )

    barrier = pltpu.get_barrier_semaphore()

    def greet(d, _):
        pl.semaphore_signal(
            barrier, inc=1, device_id={"sp": lax.rem(me + d, n)}, device_id_type=MESH
        )
        return 0

    lax.fori_loop(1, n, greet, 0)
    for d in range(1, t):
        pl.semaphore_signal(barrier, inc=1, device_id={"tp": peer_t(d)}, device_id_type=MESH)

    res_at = lambda g: res.at[g]
    ow_at = lambda g: ow.at[g]
    att_at = lambda g: att_all.at[g]

    locals_ = [
        pltpu.make_async_copy(kv_in, kv.at[aligned(me * tok, tok)], local_sem.at[0]),
        pltpu.make_async_copy(up_in, up.at[aligned(me * block, block)], local_sem.at[1]),
        pltpu.make_async_copy(down_in, down.at[aligned(me * block, block)], local_sem.at[2]),
        pltpu.make_async_copy(br_in, br.at[me], local_sem.at[3]),
        pltpu.make_async_copy(res_in, res.at[me_t], local_sem.at[4]),
        pltpu.make_async_copy(ow_in, ow.at[me_t], local_sem.at[5]),
    ]
    pl.semaphore_wait(barrier, n - 1 + t - 1)
    start_own(KV)

    def send_breaks(d, _):
        br_copy(d).start()
        return 0

    lax.fori_loop(1, n, send_breaks, 0)
    for c in locals_:
        c.start()
    for d in range(1, t):
        tp_copy(ow_in, ow_at, ow_send, ow_recv, d).start()
    for d in range(1, t):
        tp_copy(res_in, res_at, res_send, res_recv, d).start()

    key_row = lax.broadcasted_iota(jnp.int32, (tok, tok), 0)
    key_col = lax.broadcasted_iota(jnp.int32, (tok, tok), 1)
    lower[...] = jnp.where(key_row > key_col, 1.0, 0.0).astype(BF16)
    later_sum[...] = jnp.zeros_like(later_sum)
    totals[...] = jnp.zeros_like(totals)

    def kv_event(e, _):
        event(KV, e)
        return 0

    lax.fori_loop(0, n - 2, kv_event, 0)

    def last_event(item):
        ring_landed(item, RIGHT, half_n, 0).wait_recv()
        ring_landed(item, LEFT, half_n, 1).wait_recv()

    last_event(KV)

    def wait_breaks(d, _):
        br_copy(d, landed=True).wait_recv()
        return 0

    lax.fori_loop(1, n, wait_breaks, 0)
    for c in locals_:
        c.wait()

    scale = hd ** (-0.5)
    tile = 128

    def attend_block(j):
        b = me - j
        for h in range(heads):
            def rows(i, _):
                at = aligned(i * tile, tile)
                keys = kv[aligned(b * tok, tok), pl.ds(h * hd, hd)]
                vals = kv[aligned(b * tok, tok), pl.ds(width + h * hd, hd)]
                z = lax.dot_general(
                    q_ref[at, pl.ds(h * hd, hd)],
                    keys,
                    (((1,), (1,)), ((), ())),
                    preferred_element_type=F32,
                )
                z = z * scale + br[b, pl.ds(h, 1), :]
                soft = jnp.log(1.0 + jnp.exp(-jnp.abs(z)))
                log_break = jnp.minimum(z, 0.0) - soft
                r = lax.broadcasted_iota(jnp.int32, (tile, tok), 0) + i * tile + j * tok
                strict = lax.broadcasted_iota(jnp.int32, (tile, tok), 1) < r
                log_keep = jnp.where(strict, log_break - z, 0.0)
                high = log_keep.astype(BF16)
                low = (log_keep - high.astype(F32)).astype(BF16)
                tri = lower[...]
                later = jnp.dot(high, tri, preferred_element_type=F32) + jnp.dot(
                    low, tri, preferred_element_type=F32
                )
                before = later_sum[h, at, :]
                w = jnp.exp(log_break + later + before[:, 0:1])
                w = jnp.where(strict, w, 0.0).astype(BF16)
                totals[at, pl.ds(h * hd, hd)] += jnp.dot(w, vals, preferred_element_type=F32)
                later_sum[h, at, :] = before + jnp.sum(log_keep, axis=1, keepdims=True)
                return 0

            lax.fori_loop(0, tok // tile, rows, 0)

    def attend_step(j, _):
        @pl.when(j <= me)
        def _():
            attend_block(j)

        @pl.when(j < n - 2)
        def _():
            event(UP, j)

        return 0

    lax.fori_loop(0, n, attend_step, 0)

    own_att = att_all.at[me_t]
    own_att[...] = totals[...].astype(BF16)
    for d in range(1, t):
        tp_copy(own_att, att_at, att_send, att_recv, d).start()
    last_event(UP)
    for d in range(1, t):
        tp_landed(ow_at, ow_send, ow_recv, d).wait_recv()
        tp_landed(res_at, res_send, res_recv, d).wait_recv()
    for d in range(1, t):
        tp_landed(att_at, att_send, att_recv, d).wait_recv()

    big = 256

    def mix_rows(i, _):
        at = aligned(i * big, big)
        for c in range(t):
            lanes = pl.ds(c * cols, cols)
            acc = ALPHA * res[c, at, :].astype(F32)
            mixed = jnp.zeros((big, cols), F32)
            for g in range(t):
                mixed = mixed + jnp.dot(
                    att_all[g, at, :], ow[g, :, lanes], preferred_element_type=F32
                ).astype(BF16).astype(F32)
            pre[at, lanes] = acc + mixed
        return 0

    lax.fori_loop(0, tok // big, mix_rows, 0)
    event(DOWN, 0)

    small = 64

    def norm_rows(i, _):
        at = aligned(i * small, small)
        x = pre[at, :]
        center = jnp.sum(x, axis=1, keepdims=True) / feat
        x = x - center
        spread = jnp.sum(x * x, axis=1, keepdims=True) / feat
        first[at, :] = (x * lax.rsqrt(spread + EPSILON) * g1_ref[...] + b1_ref[...]).astype(BF16)
        return 0

    lax.fori_loop(0, tok // small, norm_rows, 0)

    hidden = up.shape[1]
    strip = 256

    def up_cols(i, _):
        lanes = aligned(i * strip, strip)
        a = jnp.dot(first[...], up[:, lanes], preferred_element_type=F32)
        a = jnp.maximum(a, 0.0)
        activated[:, lanes] = (a * a).astype(BF16)
        return 0

    event(DOWN, 1)
    lax.fori_loop(0, hidden // strip, up_cols, 0)

    def mix_copy(s):
        k = lax.rem(s, per)
        owner = s // per
        return owner, pltpu.make_async_remote_copy(
            src_ref=part.at[s],
            dst_ref=mix.at[me_t, k],
            send_sem=mix_send.at[s],
            recv_sem=mix_recv.at[me_t, k],
            device_id={"tp": owner},
            device_id_type=MESH,
        )

    def down_block(s):
        y = lax.dot_general(
            activated[...],
            down[aligned(s * block, block), :],
            (((1,), (1,)), ((), ())),
            preferred_element_type=F32,
        ).astype(BF16)
        owner, copy = mix_copy(s)

        @pl.when(owner == me_t)
        def _():
            mix[me_t, lax.rem(s, per)] = y

        @pl.when(owner != me_t)
        def _():
            part[s] = y
            copy.start()

    down_block(me)

    def down_step(h, _):
        @pl.when(h > 1)
        def _():
            event(DOWN, 2 * h - 2)
            event(DOWN, 2 * h - 1)

        def side(w, _):
            down_block(at_pos(pos + (2 * w - 1) * h))
            return 0

        lax.fori_loop(0, 2, side, 0)
        return 0

    lax.fori_loop(1, half_n, down_step, 0)
    last_event(DOWN)
    down_block(at_pos(pos + half_n))

    def mix_wait(s, _):
        owner, copy = mix_copy(s)

        @pl.when(owner != me_t)
        def _():
            copy.wait_send()

        return 0

    for d in range(1, t):
        g = lax.rem(me_t + t - d, t)
        for k in range(per):
            dst = mix.at[g, k]
            pltpu.make_async_remote_copy(
                src_ref=dst,
                dst_ref=dst,
                send_sem=mix_send.at[0],
                recv_sem=mix_recv.at[g, k],
                device_id={"tp": peer_t(d)},
                device_id_type=MESH,
            ).wait_recv()

    def second_pre(i, _):
        at = aligned(i * 128, 128)
        sums = jnp.zeros((128, 1), F32)
        squares = jnp.zeros((128, 1), F32)
        x = ALPHA * first[at, aligned(me_t * cols, cols)].astype(F32)
        pieces = []
        for k in range(per):
            v = mix[0, k, at, :].astype(F32)
            for g in range(1, t):
                v = v + mix[g, k, at, :].astype(F32)
            pieces.append(v)
        x = x + (jnp.concatenate(pieces, axis=1) if per > 1 else pieces[0])
        pre[at, pl.ds(0, cols)] = x
        sums = jnp.sum(x, axis=1, keepdims=True)
        squares = jnp.sum(x * x, axis=1, keepdims=True)
        lane = lax.broadcasted_iota(jnp.int32, (128, 128), 1)
        s = jnp.where(lane == 0, sums, jnp.where(lane == 1, squares, 0.0))
        stat[me_t, :, at] = s.T[0:8, :]
        return 0

    for i in range(tok // 128):
        second_pre(i, 0)
    stat_at = lambda g: stat.at[g]
    for d in range(1, t):
        tp_copy(stat.at[me_t], stat_at, stat_send, stat_recv, d).start()

    lax.fori_loop(0, n, mix_wait, 0)
    for item in (KV, UP, DOWN):
        drain_sends(item)

    def br_done(d, _):
        br_copy(d).wait_send()
        return 0

    lax.fori_loop(1, n, br_done, 0)
    for d in range(1, t):
        tp_copy(ow_in, ow_at, ow_send, ow_recv, d).wait_send()
        tp_copy(res_in, res_at, res_send, res_recv, d).wait_send()
        tp_copy(own_att, att_at, att_send, att_recv, d).wait_send()
    for d in range(1, t):
        tp_landed(stat_at, stat_send, stat_recv, d).wait_recv()

    for i in range(tok // 128):
        at = pl.ds(i * 128, 128)
        s = stat[0, :, at]
        for g in range(1, t):
            s = s + stat[g, :, at]
        s = jnp.concatenate([s, jnp.zeros((120, 128), F32)], axis=0).T
        center = s[:, 0:1] / feat
        spread = s[:, 1:2] / feat - center * center
        x = pre[at, pl.ds(0, cols)]
        x = (x - center) * lax.rsqrt(spread + EPSILON)
        out_ref[at, :] = (x * g2_ref[me_t] + b2_ref[me_t]).astype(BF16)
    for d in range(1, t):
        tp_copy(stat.at[me_t], stat_at, stat_send, stat_recv, d).wait_send()


def solution(mesh):
    n, t = mesh.shape["sp"], mesh.shape["tp"]

    def body(
        queries,
        keys,
        values,
        breaks,
        residual_in,
        out_weight,
        first_gain,
        first_shift,
        up_weight,
        down_weight,
        second_gain,
        second_shift,
    ):
        tok, width = queries.shape
        heads = breaks.shape[1]
        feat = out_weight.shape[1]
        cols = residual_in.shape[1]
        hidden = up_weight.shape[1]
        block = up_weight.shape[0]
        per = n // t
        kv = jnp.concatenate([keys, values], axis=1)
        br = jnp.pad(breaks.astype(F32).T, ((0, 8 - heads), (0, 0)))
        any_ = pl.BlockSpec(memory_space=pl.ANY)
        vmem = pl.BlockSpec(memory_space=pltpu.VMEM)
        dma = pltpu.SemaphoreType.DMA
        ring = dma((3, 2, n // 2 + 1, 2))
        return pl.pallas_call(
            functools.partial(layer_kernel, n, t, heads),
            out_shape=jax.ShapeDtypeStruct((tok, cols), BF16),
            in_specs=[vmem, any_, any_, any_, any_, vmem, vmem, any_, any_, vmem, vmem],
            out_specs=vmem,
            scratch_shapes=[
                pltpu.VMEM((n * tok, 2 * width), BF16),
                pltpu.VMEM((feat, hidden), BF16),
                pltpu.VMEM((feat, hidden), BF16),
                pltpu.VMEM((n, 8, tok), F32),
                pltpu.VMEM((t, width, feat), BF16),
                pltpu.VMEM((t, tok, cols), BF16),
                pltpu.VMEM((heads, tok, 128), F32),
                pltpu.VMEM((tok, width), F32),
                pltpu.VMEM((t, tok, width), BF16),
                pltpu.VMEM((tok, tok), BF16),
                pltpu.VMEM((tok, feat), F32),
                pltpu.VMEM((tok, feat), BF16),
                pltpu.VMEM((tok, hidden), BF16),
                pltpu.VMEM((n, tok, block), BF16),
                pltpu.VMEM((t, per, tok, block), BF16),
                pltpu.VMEM((t, 8, tok), F32),
                ring,
                ring,
                dma((n,)),
                dma((n,)),
                dma((t,)),
                dma((t,)),
                dma((t,)),
                dma((t,)),
                dma((t,)),
                dma((t,)),
                dma((n,)),
                dma((t, per)),
                dma((t,)),
                dma((t,)),
                dma((6,)),
            ],
            compiler_params=pltpu.CompilerParams(
                collective_id=0, has_side_effects=True, vmem_limit_bytes=62 * 1024 * 1024
            ),
        )(
            queries,
            kv,
            br,
            residual_in,
            out_weight,
            first_gain.reshape(1, feat),
            first_shift.reshape(1, feat),
            up_weight,
            down_weight,
            second_gain.reshape(t, 1, cols),
            second_shift.reshape(t, 1, cols),
        )

    return jax.shard_map(
        body,
        mesh=mesh,
        in_specs=(
            P("sp", "tp"),
            P("sp", "tp"),
            P("sp", "tp"),
            P("sp", "tp"),
            P("sp", "tp"),
            P("tp", None),
            P(),
            P(),
            P("sp", "tp"),
            P("sp", "tp"),
            P(),
            P(),
        ),
        out_specs=P("sp", "tp"),
        check_vma=False,
    )
```

```python
import functools

import jax
import jax.numpy as jnp
from jax import lax
from jax.experimental import pallas as pl
from jax.experimental.pallas import tpu as pltpu
from jax.sharding import PartitionSpec as P

ALPHA = 2.0**0.25
EPSILON = 1e-05
MESH = pl.DeviceIdType.MESH
F32 = jnp.float32
BF16 = jnp.bfloat16
KV, UP, DOWN = 0, 1, 2


def aligned(start, size):
    return pl.ds(pl.multiple_of(start, size), size)


def layer_kernel(
    n,
    t,
    heads,
    q_ref,
    kv_in,
    br_in,
    res_in,
    ow_in,
    g1_ref,
    b1_ref,
    up_in,
    down_in,
    g2_ref,
    b2_ref,
    out_ref,
    kv,
    up,
    down,
    br,
    ow,
    res,
    later_sum,
    totals,
    att_all,
    lower,
    pre,
    first,
    activated,
    part,
    mix,
    stat,
    up_send,
    up_recv,
    down_send,
    down_recv,
    cross_send,
    cross_recv,
    kvx_send,
    kvx_recv,
    br_send,
    br_recv,
    spread_send,
    spread_recv,
    quarter_send,
    quarter_recv,
    mix_send,
    mix_recv,
    stat_send,
    stat_recv,
    local_sem,
):
    me = lax.axis_index("sp")
    me_t = lax.axis_index("tp")
    tok = q_ref.shape[0]
    width = q_ref.shape[1]
    hd = width // heads
    feat = first.shape[2]
    cols = feat // t
    block = feat // n
    per = n // t
    layers = n // 2
    part_hidden = up.shape[1]
    z, y = me // 2, lax.rem(me, 2)
    partner = 2 * z + 1 - y
    x_count = t // 2
    x, core = me_t // 2, lax.rem(me_t, 2)
    half = tok // 2
    full = (kv, up, down)
    own_in = (kv_in, up_in, down_in)

    def remote(src, dst, send, recv, sp=None, tp=None):
        where = {}
        if sp is not None:
            where["sp"] = sp
        if tp is not None:
            where["tp"] = tp
        return pltpu.make_async_remote_copy(
            src_ref=src,
            dst_ref=dst,
            send_sem=send,
            recv_sem=recv,
            device_id=where,
            device_id_type=MESH,
        )

    def slot(item, layer, piece):
        source = 2 * layer + (y if piece == 0 else 1 - y)
        if item == KV:
            return kv.at[aligned(source * tok + y * half, half)]
        return full[item].at[aligned(source * block, block)]

    def own_piece(item):
        if item == KV:
            return kv_in.at[aligned(y * half, half)]
        return own_in[item].at[:, aligned(y * part_hidden, part_hidden)]

    def climb(item, hop, piece, own=False):
        dst = slot(item, z + 1 - hop, piece)
        return remote(
            own_piece(item) if own else dst,
            dst,
            up_send.at[item, hop, piece],
            up_recv.at[item, hop, piece],
            sp=lax.rem(me + 2, n),
        )

    def climbed(item, hop, piece):
        dst = slot(item, z - hop, piece)
        return remote(
            dst, dst, up_send.at[item, hop, piece], up_recv.at[item, hop, piece], sp=lax.rem(me + 2, n)
        )

    def sink(item, hop, piece, own=False):
        dst = slot(item, z - 1 + hop, piece)
        return remote(
            own_piece(item) if own else dst,
            dst,
            down_send.at[item, hop, piece],
            down_recv.at[item, hop, piece],
            sp=lax.rem(me + n - 2, n),
        )

    def sunk(item, hop, piece):
        dst = slot(item, z + hop, piece)
        return remote(
            dst,
            dst,
            down_send.at[item, hop, piece],
            down_recv.at[item, hop, piece],
            sp=lax.rem(me + n - 2, n),
        )

    def cross(item, landed=False):
        source = partner if landed else me
        dst = full[item].at[aligned(source * block, block)]
        src = own_in[item].at[:, aligned((1 - y) * part_hidden, part_hidden)]
        return remote(dst if landed else src, dst, cross_send.at[item], cross_recv.at[item], sp=partner)

    def cross_kv(which, landed=False):
        source = partner if landed else me
        receiver_y = y if landed else 1 - y
        h = receiver_y if which == 0 else 1 - receiver_y
        dst = kv.at[aligned(source * tok + h * half, half)]
        src = dst if landed else kv_in.at[aligned(h * half, half)]
        return remote(src, dst, kvx_send.at[0, which], kvx_recv.at[0, which], sp=partner)

    def cross_kv_hop(hop, piece, landed=False):
        if landed:
            source = 2 * (z - hop) + (1 - y if piece == 0 else y)
            dst = kv.at[aligned(source * tok + (1 - y) * half, half)]
        else:
            dst = slot(KV, z - hop, piece)
        return remote(dst, dst, kvx_send.at[hop, piece], kvx_recv.at[hop, piece], sp=partner)

    can_up = z + 1 < layers
    can_down = z > 0

    def start_up(item):
        @pl.when(can_up)
        def _():
            climb(item, 1, 0, own=True).start()
            climb(item, 1, 1).start()

    def start_down(item):
        @pl.when(can_down)
        def _():
            sink(item, 1, 0, own=True).start()
            sink(item, 1, 1).start()

    def kv_hop(hop):
        for piece in range(2):

            @pl.when(z - hop >= 0)
            def _():
                climbed(KV, hop, piece).wait_recv()

                @pl.when(can_up)
                def _():
                    climb(KV, hop + 1, piece).start()

                cross_kv_hop(hop, piece).start()

    def event(item, hop, piece):
        @pl.when(z - hop >= 0)
        def _():
            climbed(item, hop, piece).wait_recv()

            @pl.when(can_up)
            def _():
                climb(item, hop + 1, piece).start()

        @pl.when(z + hop < layers)
        def _():
            sunk(item, hop, piece).wait_recv()

            @pl.when(can_down)
            def _():
                sink(item, hop + 1, piece).start()

    def drain_sends(item):
        def one(hop, _):
            for piece in range(2):

                @pl.when(jnp.logical_and(can_up, z + 1 - hop >= 0))
                def _():
                    climb(item, hop, piece).wait_send()

                if item != KV:

                    @pl.when(jnp.logical_and(can_down, z - 1 + hop < layers))
                    def _():
                        sink(item, hop, piece).wait_send()
                else:

                    @pl.when(z - hop >= 0)
                    def _():
                        cross_kv_hop(hop, piece).wait_send()

            return 0

        lax.fori_loop(1, layers, one, 0)

    def spread_copy(kind, at, stage, d, src=None):
        if stage == 0:
            dst = at(me_t)
            to = lax.rem(x + d, x_count) * 2 + core
            i = d
        else:
            dst = at(lax.rem(x + x_count - d, x_count) * 2 + core)
            to = x * 2 + 1 - core
            i = x_count + d
        return remote(
            dst if src is None else src, dst, spread_send.at[kind, i], spread_recv.at[kind, i], tp=to
        )

    def spread_landed(kind, at, stage, d):
        if stage == 0:
            dst = at(lax.rem(x + x_count - d, x_count) * 2 + core)
            to = lax.rem(x + d, x_count) * 2 + core
            i = d
        else:
            dst = at(lax.rem(x + x_count - d, x_count) * 2 + 1 - core)
            to = x * 2 + 1 - core
            i = x_count + d
        return remote(dst, dst, spread_send.at[kind, i], spread_recv.at[kind, i], tp=to)

    def spread_start(kind, at, src=None):
        for d in range(1, x_count):
            spread_copy(kind, at, 0, d, src).start()
        spread_copy(kind, at, 1, 0, src).start()

    def spread_forward(kind, at):
        for d in range(1, x_count):
            spread_landed(kind, at, 0, d).wait_recv()
            spread_copy(kind, at, 1, d).start()

    def spread_finish(kind, at):
        for d in range(x_count):
            spread_landed(kind, at, 1, d).wait_recv()

    def spread_drain(kind, at):
        for d in range(1, x_count):
            spread_copy(kind, at, 0, d).wait_send()
        for d in range(x_count):
            spread_copy(kind, at, 1, d).wait_send()

    OW, RES, ATT, FIRST = range(4)
    ow_at = lambda g: ow.at[g]
    res_at = lambda g: res.at[g]
    att_at = lambda g: att_all.at[g]
    far_at = lambda g: first.at[1 - y, :, aligned(g * cols, cols)]

    def peer_t(d):
        return lax.rem(me_t + d, t)

    def br_copy(d, landed=False):
        owner = lax.rem(me + n - d, n) if landed else me
        return remote(
            br.at[owner] if landed else br_in,
            br.at[owner],
            br_send.at[d],
            br_recv.at[d],
            sp=lax.rem(me + d, n),
        )

    barrier = pltpu.get_barrier_semaphore()

    def greet(d, _):
        pl.semaphore_signal(
            barrier, inc=1, device_id={"sp": lax.rem(me + d, n)}, device_id_type=MESH
        )
        return 0

    lax.fori_loop(1, n, greet, 0)
    for d in range(1, t):
        pl.semaphore_signal(barrier, inc=1, device_id={"tp": peer_t(d)}, device_id_type=MESH)
        pl.semaphore_signal(
            barrier, inc=1, device_id={"sp": partner, "tp": peer_t(d)}, device_id_type=MESH
        )

    own_half = aligned(y * part_hidden, part_hidden)
    locals_ = [
        pltpu.make_async_copy(kv_in, kv.at[aligned(me * tok, tok)], local_sem.at[0]),
        pltpu.make_async_copy(
            up_in.at[:, own_half], up.at[aligned(me * block, block)], local_sem.at[1]
        ),
        pltpu.make_async_copy(
            down_in.at[:, own_half], down.at[aligned(me * block, block)], local_sem.at[2]
        ),
        pltpu.make_async_copy(br_in, br.at[me], local_sem.at[3]),
        pltpu.make_async_copy(res_in, res.at[me_t], local_sem.at[4]),
        pltpu.make_async_copy(ow_in, ow.at[me_t], local_sem.at[5]),
    ]
    pl.semaphore_wait(barrier, n - 1 + 2 * (t - 1))

    @pl.when(can_up)
    def _():
        climb(KV, 1, 0, own=True).start()

    cross_kv(0).start()

    @pl.when(can_down)
    def _():
        sink(UP, 1, 0, own=True).start()

    cross_kv(1).start()
    cross(UP).start()
    cross(DOWN).start()

    def send_breaks(d, _):
        br_copy(d).start()
        return 0

    lax.fori_loop(1, n, send_breaks, 0)
    for c in locals_:
        c.start()
    spread_start(RES, res_at, res_in)
    spread_start(OW, ow_at, ow_in)

    key_row = lax.broadcasted_iota(jnp.int32, (tok, tok), 0)
    key_col = lax.broadcasted_iota(jnp.int32, (tok, tok), 1)
    lower[...] = jnp.where(key_row > key_col, 1.0, 0.0).astype(BF16)
    later_sum[...] = jnp.zeros_like(later_sum)
    totals[...] = jnp.zeros_like(totals)

    cross_kv(0, landed=True).wait_recv()

    @pl.when(can_up)
    def _():
        climb(KV, 1, 1).start()

    cross_kv(1, landed=True).wait_recv()
    cross(UP, landed=True).wait_recv()

    @pl.when(can_down)
    def _():
        sink(UP, 1, 1).start()

    def kv_event(hop, _):
        @pl.when(hop == layers - 1)
        def _():
            start_up(UP)

        kv_hop(hop)
        return 0

    lax.fori_loop(1, layers, kv_event, 0)
    spread_forward(RES, res_at)
    spread_forward(OW, ow_at)

    def kv_rest(hop, _):
        for piece in range(2):

            @pl.when(z - hop >= 0)
            def _():
                cross_kv_hop(hop, piece, landed=True).wait_recv()

        return 0

    lax.fori_loop(1, layers, kv_rest, 0)

    def wait_breaks(d, _):
        br_copy(d, landed=True).wait_recv()
        return 0

    lax.fori_loop(1, n, wait_breaks, 0)
    for c in locals_:
        c.wait()
    cross(DOWN, landed=True).wait_recv()

    scale = hd ** (-0.5)
    tile = 128

    def attend_block(j):
        b = me - j
        for h in range(heads):
            def rows(i, _):
                at = aligned(i * tile, tile)
                keys = kv[aligned(b * tok, tok), pl.ds(h * hd, hd)]
                vals = kv[aligned(b * tok, tok), pl.ds(width + h * hd, hd)]
                z = lax.dot_general(
                    q_ref[at, pl.ds(h * hd, hd)],
                    keys,
                    (((1,), (1,)), ((), ())),
                    preferred_element_type=F32,
                )
                z = z * scale + br[b, pl.ds(h, 1), :]
                soft = jnp.log(1.0 + jnp.exp(-jnp.abs(z)))
                log_break = jnp.minimum(z, 0.0) - soft
                r = lax.broadcasted_iota(jnp.int32, (tile, tok), 0) + i * tile + j * tok
                strict = lax.broadcasted_iota(jnp.int32, (tile, tok), 1) < r
                log_keep = jnp.where(strict, log_break - z, 0.0)
                high = log_keep.astype(BF16)
                low = (log_keep - high.astype(F32)).astype(BF16)
                tri = lower[...]
                later = jnp.dot(high, tri, preferred_element_type=F32) + jnp.dot(
                    low, tri, preferred_element_type=F32
                )
                before = later_sum[h, at, :]
                w = jnp.exp(log_break + later + before[:, 0:1])
                w = jnp.where(strict, w, 0.0).astype(BF16)
                totals[at, pl.ds(h * hd, hd)] += jnp.dot(w, vals, preferred_element_type=F32)
                later_sum[h, at, :] = before + jnp.sum(log_keep, axis=1, keepdims=True)
                return 0

            lax.fori_loop(0, tok // tile, rows, 0)

    def up_event(e):
        hop = 1 + e // 2
        for piece in range(2):

            @pl.when(lax.rem(e, 2) == piece)
            def _():
                event(UP, hop, piece)

        @pl.when(e == 2 * layers - 4)
        def _():
            start_up(DOWN)
            start_down(DOWN)

    def attend_step(j, _):
        @pl.when(j <= me)
        def _():
            attend_block(j)

        @pl.when(j < 2 * layers - 2)
        def _():
            up_event(j)

        return 0

    lax.fori_loop(0, n, attend_step, 0)

    att_all[me_t] = totals[...].astype(BF16)
    spread_start(ATT, att_at)
    spread_finish(OW, ow_at)
    spread_finish(RES, res_at)
    spread_forward(ATT, att_at)
    spread_finish(ATT, att_at)

    big = 256

    def mix_rows(i, _):
        at = aligned(i * big, big)
        for c in range(t):
            lanes = pl.ds(c * cols, cols)
            acc = ALPHA * res[c, at, :].astype(F32)
            mixed = jnp.zeros((big, cols), F32)
            for g in range(t):
                mixed = mixed + jnp.dot(
                    att_all[g, at, :], ow[g, :, lanes], preferred_element_type=F32
                ).astype(BF16).astype(F32)
            pre[at, lanes] = acc + mixed
        return 0

    lax.fori_loop(0, tok // big, mix_rows, 0)

    small = 64

    def norm_rows(i, _):
        at = aligned(i * small, small)
        v = pre[at, :]
        center = jnp.sum(v, axis=1, keepdims=True) / feat
        v = v - center
        spread = jnp.sum(v * v, axis=1, keepdims=True) / feat
        first[y, at, :] = (v * lax.rsqrt(spread + EPSILON) * g1_ref[...] + b1_ref[...]).astype(BF16)
        return 0

    lax.fori_loop(0, tok // small, norm_rows, 0)

    def quarter(landed=False):
        dst = first.at[1 - y if landed else y, :, aligned(me_t * cols, cols)]
        return remote(dst, dst, quarter_send.at[0], quarter_recv.at[0], sp=partner)

    quarter().start()
    event(DOWN, 1, 0)

    strip = 256

    def up_side(a):
        def up_cols(i, _):
            lanes = aligned(i * strip, strip)
            v = jnp.dot(first[a], up[:, lanes], preferred_element_type=F32)
            v = jnp.maximum(v, 0.0)
            activated[a, :, lanes] = (v * v).astype(BF16)
            return 0

        lax.fori_loop(0, part_hidden // strip, up_cols, 0)

    up_side(y)
    quarter(landed=True).wait_recv()
    spread_start(FIRST, far_at)
    event(DOWN, 1, 1)
    spread_forward(FIRST, far_at)
    spread_finish(FIRST, far_at)
    up_side(1 - y)

    def mix_copy(s, a):
        k = lax.rem(s, per)
        owner = s // per
        return owner, remote(
            part.at[s, a],
            mix.at[y * t + me_t, k],
            mix_send.at[s, a],
            mix_recv.at[y * t + me_t, k],
            sp=2 * z + a,
            tp=owner,
        )

    def down_block(s):
        def side(i, _):
            a = lax.rem(y + 1 + i, 2)
            v = lax.dot_general(
                activated[a],
                down[aligned(s * block, block), :],
                (((1,), (1,)), ((), ())),
                preferred_element_type=F32,
            ).astype(BF16)
            owner, copy = mix_copy(s, a)
            mine = jnp.logical_and(owner == me_t, a == y)

            @pl.when(mine)
            def _():
                mix[y * t + me_t, lax.rem(s, per)] = v

            @pl.when(jnp.logical_not(mine))
            def _():
                part[s, a] = v
                copy.start()

            return 0

        lax.fori_loop(0, 2, side, 0)

    down_block(me)
    down_block(partner)

    def down_step(hop, _):
        for piece in range(2):

            @pl.when(hop > 1)
            def _():
                event(DOWN, hop, piece)

            c = y if piece == 0 else 1 - y

            @pl.when(z - hop >= 0)
            def _():
                down_block(2 * (z - hop) + c)

            @pl.when(z + hop < layers)
            def _():
                down_block(2 * (z + hop) + c)

        return 0

    lax.fori_loop(1, layers, down_step, 0)

    def mix_wait(s, _):
        for a in range(2):
            owner, copy = mix_copy(s, a)

            @pl.when(jnp.logical_not(jnp.logical_and(owner == me_t, a == y)))
            def _():
                copy.wait_send()

        return 0

    def mix_landed(g, k):
        dst = mix.at[g, k]
        remote(dst, dst, mix_send.at[0, 0], mix_recv.at[g, k], sp=partner).wait_recv()

    for k in range(per):
        for d in range(1, t):
            mix_landed(y * t + lax.rem(me_t + t - d, t), k)
        for d in range(t):
            mix_landed((1 - y) * t + lax.rem(me_t + t - d, t), k)

    for i in range(tok // 128):
        at = pl.ds(i * 128, 128)
        v = ALPHA * first[y, at, aligned(me_t * cols, cols)].astype(F32)
        pieces = []
        for k in range(per):
            u = mix[0, k, at, :].astype(F32)
            for g in range(1, 2 * t):
                u = u + mix[g, k, at, :].astype(F32)
            pieces.append(u)
        v = v + (jnp.concatenate(pieces, axis=1) if per > 1 else pieces[0])
        pre[at, pl.ds(0, cols)] = v
        sums = jnp.sum(v, axis=1, keepdims=True)
        squares = jnp.sum(v * v, axis=1, keepdims=True)
        lane = lax.broadcasted_iota(jnp.int32, (128, 128), 1)
        both = jnp.where(lane == 0, sums, jnp.where(lane == 1, squares, 0.0))
        stat[me_t, :, at] = both.T[0:8, :]

    def stat_copy(d, landed=False):
        dst = stat.at[lax.rem(me_t + t - d, t) if landed else me_t]
        return remote(dst, dst, stat_send.at[d], stat_recv.at[d], tp=peer_t(d))

    for d in range(1, t):
        stat_copy(d).start()

    lax.fori_loop(0, n, mix_wait, 0)
    for item in (KV, UP, DOWN):
        drain_sends(item)
    cross_kv(0).wait_send()
    cross_kv(1).wait_send()
    cross(UP).wait_send()
    cross(DOWN).wait_send()
    quarter().wait_send()

    def br_done(d, _):
        br_copy(d).wait_send()
        return 0

    lax.fori_loop(1, n, br_done, 0)
    spread_drain(OW, ow_at)
    spread_drain(RES, res_at)
    spread_drain(ATT, att_at)
    spread_drain(FIRST, far_at)
    for d in range(1, t):
        stat_copy(d, landed=True).wait_recv()

    for i in range(tok // 128):
        at = pl.ds(i * 128, 128)
        v = stat[0, :, at]
        for g in range(1, t):
            v = v + stat[g, :, at]
        v = jnp.concatenate([v, jnp.zeros((120, 128), F32)], axis=0).T
        center = v[:, 0:1] / feat
        spread = v[:, 1:2] / feat - center * center
        u = (pre[at, pl.ds(0, cols)] - center) * lax.rsqrt(spread + EPSILON)
        out_ref[at, :] = (u * g2_ref[me_t] + b2_ref[me_t]).astype(BF16)
    for d in range(1, t):
        stat_copy(d).wait_send()


def solution(mesh):
    n, t = mesh.shape["sp"], mesh.shape["tp"]

    def body(
        queries,
        keys,
        values,
        breaks,
        residual_in,
        out_weight,
        first_gain,
        first_shift,
        up_weight,
        down_weight,
        second_gain,
        second_shift,
    ):
        tok, width = queries.shape
        heads = breaks.shape[1]
        feat = out_weight.shape[1]
        cols = residual_in.shape[1]
        hidden = up_weight.shape[1]
        block = up_weight.shape[0]
        per = n // t
        kv = jnp.concatenate([keys, values], axis=1)
        br = jnp.pad(breaks.astype(F32).T, ((0, 8 - heads), (0, 0)))
        any_ = pl.BlockSpec(memory_space=pl.ANY)
        vmem = pl.BlockSpec(memory_space=pltpu.VMEM)
        dma = pltpu.SemaphoreType.DMA
        ring = dma((3, n // 2 + 1, 2))
        return pl.pallas_call(
            functools.partial(layer_kernel, n, t, heads),
            out_shape=jax.ShapeDtypeStruct((tok, cols), BF16),
            in_specs=[vmem, any_, any_, any_, any_, vmem, vmem, any_, any_, vmem, vmem],
            out_specs=vmem,
            scratch_shapes=[
                pltpu.VMEM((n * tok, 2 * width), BF16),
                pltpu.VMEM((feat, hidden // 2), BF16),
                pltpu.VMEM((feat, hidden // 2), BF16),
                pltpu.VMEM((n, 8, tok), F32),
                pltpu.VMEM((t, width, feat), BF16),
                pltpu.VMEM((t, tok, cols), BF16),
                pltpu.VMEM((heads, tok, 128), F32),
                pltpu.VMEM((tok, width), F32),
                pltpu.VMEM((t, tok, width), BF16),
                pltpu.VMEM((tok, tok), BF16),
                pltpu.VMEM((tok, feat), F32),
                pltpu.VMEM((2, tok, feat), BF16),
                pltpu.VMEM((2, tok, hidden // 2), BF16),
                pltpu.VMEM((n, 2, tok, block), BF16),
                pltpu.VMEM((2 * t, per, tok, block), BF16),
                pltpu.VMEM((t, 8, tok), F32),
                ring,
                ring,
                ring,
                ring,
                dma((3,)),
                dma((3,)),
                dma((n // 2, 2)),
                dma((n // 2, 2)),
                dma((n,)),
                dma((n,)),
                dma((4, t)),
                dma((4, t)),
                dma((1,)),
                dma((1,)),
                dma((n, 2)),
                dma((2 * t, per)),
                dma((t,)),
                dma((t,)),
                dma((6,)),
            ],
            compiler_params=pltpu.CompilerParams(
                collective_id=0, has_side_effects=True, vmem_limit_bytes=62 * 1024 * 1024
            ),
        )(
            queries,
            kv,
            br,
            residual_in,
            out_weight,
            first_gain.reshape(1, feat),
            first_shift.reshape(1, feat),
            up_weight,
            down_weight,
            second_gain.reshape(t, 1, cols),
            second_shift.reshape(t, 1, cols),
        )

    return jax.shard_map(
        body,
        mesh=mesh,
        in_specs=(
            P("sp", "tp"),
            P("sp", "tp"),
            P("sp", "tp"),
            P("sp", "tp"),
            P("sp", "tp"),
            P("tp", None),
            P(),
            P(),
            P("sp", "tp"),
            P("sp", "tp"),
            P(),
            P(),
        ),
        out_specs=P("sp", "tp"),
        check_vma=False,
    )
```

```python
import functools

import jax
import jax.numpy as jnp
from jax import lax
from jax.experimental import pallas as pl
from jax.experimental.pallas import tpu as pltpu
from jax.sharding import PartitionSpec as P

ALPHA = 2.0**0.25
EPSILON = 1e-05
MESH = pl.DeviceIdType.MESH
F32 = jnp.float32
BF16 = jnp.bfloat16
KV, UP, DOWN = 0, 1, 2


def aligned(start, size):
    return pl.ds(pl.multiple_of(start, size), size)


def layer_kernel(
    n,
    t,
    heads,
    q_ref,
    kv_in,
    br_in,
    res_in,
    ow_in,
    g1_ref,
    b1_ref,
    up_in,
    down_in,
    g2_ref,
    b2_ref,
    out_ref,
    kv,
    up,
    down,
    br,
    ow,
    res,
    later_sum,
    totals,
    att_all,
    lower,
    pre,
    first,
    activated,
    part,
    mix,
    stat,
    up_send,
    up_recv,
    down_send,
    down_recv,
    cross_send,
    cross_recv,
    kvx_send,
    kvx_recv,
    br_send,
    br_recv,
    spread_send,
    spread_recv,
    quarter_send,
    quarter_recv,
    mix_send,
    mix_recv,
    stat_send,
    stat_recv,
    local_sem,
):
    me = lax.axis_index("sp")
    me_t = lax.axis_index("tp")
    tok = q_ref.shape[0]
    width = q_ref.shape[1]
    hd = width // heads
    feat = first.shape[2]
    cols = feat // t
    block = feat // n
    per = n // t
    layers = n // 2
    part_hidden = up.shape[1]
    z, y = me // 2, lax.rem(me, 2)
    partner = 2 * z + 1 - y
    x_count = t // 2
    x, core = me_t // 2, lax.rem(me_t, 2)
    half = tok // 2
    full = (kv, up, down)
    own_in = (kv_in, up_in, down_in)

    def remote(src, dst, send, recv, sp=None, tp=None):
        where = {}
        if sp is not None:
            where["sp"] = sp
        if tp is not None:
            where["tp"] = tp
        return pltpu.make_async_remote_copy(
            src_ref=src,
            dst_ref=dst,
            send_sem=send,
            recv_sem=recv,
            device_id=where,
            device_id_type=MESH,
        )

    def slot(item, layer, piece):
        source = 2 * layer + (y if piece == 0 else 1 - y)
        if item == KV:
            return kv.at[aligned(source * tok + y * half, half)]
        return full[item].at[aligned(source * block, block)]

    def own_piece(item):
        if item == KV:
            return kv_in.at[aligned(y * half, half)]
        return own_in[item].at[:, aligned(y * part_hidden, part_hidden)]

    def climb(item, hop, piece, own=False):
        dst = slot(item, z + 1 - hop, piece)
        return remote(
            own_piece(item) if own else dst,
            dst,
            up_send.at[item, hop, piece],
            up_recv.at[item, hop, piece],
            sp=lax.rem(me + 2, n),
        )

    def climbed(item, hop, piece):
        dst = slot(item, z - hop, piece)
        return remote(
            dst, dst, up_send.at[item, hop, piece], up_recv.at[item, hop, piece], sp=lax.rem(me + 2, n)
        )

    def sink(item, hop, piece, own=False):
        dst = slot(item, z - 1 + hop, piece)
        return remote(
            own_piece(item) if own else dst,
            dst,
            down_send.at[item, hop, piece],
            down_recv.at[item, hop, piece],
            sp=lax.rem(me + n - 2, n),
        )

    def sunk(item, hop, piece):
        dst = slot(item, z + hop, piece)
        return remote(
            dst,
            dst,
            down_send.at[item, hop, piece],
            down_recv.at[item, hop, piece],
            sp=lax.rem(me + n - 2, n),
        )

    def cross(item, landed=False):
        source = partner if landed else me
        dst = full[item].at[aligned(source * block, block)]
        src = own_in[item].at[:, aligned((1 - y) * part_hidden, part_hidden)]
        return remote(dst if landed else src, dst, cross_send.at[item], cross_recv.at[item], sp=partner)

    def cross_kv(which, landed=False):
        source = partner if landed else me
        receiver_y = y if landed else 1 - y
        h = receiver_y if which == 0 else 1 - receiver_y
        dst = kv.at[aligned(source * tok + h * half, half)]
        src = dst if landed else kv_in.at[aligned(h * half, half)]
        return remote(src, dst, kvx_send.at[0, which], kvx_recv.at[0, which], sp=partner)

    def cross_kv_hop(hop, piece, landed=False):
        if landed:
            source = 2 * (z - hop) + (1 - y if piece == 0 else y)
            dst = kv.at[aligned(source * tok + (1 - y) * half, half)]
        else:
            dst = slot(KV, z - hop, piece)
        return remote(dst, dst, kvx_send.at[hop, piece], kvx_recv.at[hop, piece], sp=partner)

    can_up = z + 1 < layers
    can_down = z > 0

    def start_up(item):
        @pl.when(can_up)
        def _():
            climb(item, 1, 0, own=True).start()
            climb(item, 1, 1).start()

    def start_down(item):
        @pl.when(can_down)
        def _():
            sink(item, 1, 0, own=True).start()
            sink(item, 1, 1).start()

    def kv_hop(hop):
        for piece in range(2):

            @pl.when(z - hop >= 0)
            def _():
                climbed(KV, hop, piece).wait_recv()

                @pl.when(can_up)
                def _():
                    climb(KV, hop + 1, piece).start()

                cross_kv_hop(hop, piece).start()

    def event(item, hop, piece):
        @pl.when(z - hop >= 0)
        def _():
            climbed(item, hop, piece).wait_recv()

            @pl.when(can_up)
            def _():
                climb(item, hop + 1, piece).start()

        @pl.when(z + hop < layers)
        def _():
            sunk(item, hop, piece).wait_recv()

            @pl.when(can_down)
            def _():
                sink(item, hop + 1, piece).start()

    def drain_sends(item):
        def one(hop, _):
            for piece in range(2):

                @pl.when(jnp.logical_and(can_up, z + 1 - hop >= 0))
                def _():
                    climb(item, hop, piece).wait_send()

                if item != KV:

                    @pl.when(jnp.logical_and(can_down, z - 1 + hop < layers))
                    def _():
                        sink(item, hop, piece).wait_send()
                else:

                    @pl.when(z - hop >= 0)
                    def _():
                        cross_kv_hop(hop, piece).wait_send()

            return 0

        lax.fori_loop(1, layers, one, 0)

    def spread_copy(kind, at, stage, d, src=None):
        if stage == 0:
            dst = at(me_t)
            to = lax.rem(x + d, x_count) * 2 + core
            i = d
        else:
            dst = at(lax.rem(x + x_count - d, x_count) * 2 + core)
            to = x * 2 + 1 - core
            i = x_count + d
        return remote(
            dst if src is None else src, dst, spread_send.at[kind, i], spread_recv.at[kind, i], tp=to
        )

    def spread_landed(kind, at, stage, d):
        if stage == 0:
            dst = at(lax.rem(x + x_count - d, x_count) * 2 + core)
            to = lax.rem(x + d, x_count) * 2 + core
            i = d
        else:
            dst = at(lax.rem(x + x_count - d, x_count) * 2 + 1 - core)
            to = x * 2 + 1 - core
            i = x_count + d
        return remote(dst, dst, spread_send.at[kind, i], spread_recv.at[kind, i], tp=to)

    def spread_start(kind, at, src=None):
        for d in range(1, x_count):
            spread_copy(kind, at, 0, d, src).start()
        spread_copy(kind, at, 1, 0, src).start()

    def spread_forward(kind, at):
        for d in range(1, x_count):
            spread_landed(kind, at, 0, d).wait_recv()
            spread_copy(kind, at, 1, d).start()

    def spread_finish(kind, at):
        for d in range(x_count):
            spread_landed(kind, at, 1, d).wait_recv()

    def spread_drain(kind, at):
        for d in range(1, x_count):
            spread_copy(kind, at, 0, d).wait_send()
        for d in range(x_count):
            spread_copy(kind, at, 1, d).wait_send()

    OW, RES, ATT, FIRST = range(4)
    ow_at = lambda g: ow.at[g]
    res_at = lambda g: res.at[g]
    att_at = lambda g: att_all.at[g]
    far_at = lambda g: first.at[1 - y, :, aligned(g * cols, cols)]

    def peer_t(d):
        return lax.rem(me_t + d, t)

    def br_copy(d, landed=False):
        owner = lax.rem(me + n - d, n) if landed else me
        return remote(
            br.at[owner] if landed else br_in,
            br.at[owner],
            br_send.at[d],
            br_recv.at[d],
            sp=lax.rem(me + d, n),
        )

    barrier = pltpu.get_barrier_semaphore()

    def greet(d, _):
        pl.semaphore_signal(
            barrier, inc=1, device_id={"sp": lax.rem(me + d, n)}, device_id_type=MESH
        )
        return 0

    lax.fori_loop(1, n, greet, 0)
    for d in range(1, t):
        pl.semaphore_signal(barrier, inc=1, device_id={"tp": peer_t(d)}, device_id_type=MESH)
        pl.semaphore_signal(
            barrier, inc=1, device_id={"sp": partner, "tp": peer_t(d)}, device_id_type=MESH
        )

    own_half = aligned(y * part_hidden, part_hidden)
    locals_ = [
        pltpu.make_async_copy(kv_in, kv.at[aligned(me * tok, tok)], local_sem.at[0]),
        pltpu.make_async_copy(
            up_in.at[:, own_half], up.at[aligned(me * block, block)], local_sem.at[1]
        ),
        pltpu.make_async_copy(
            down_in.at[:, own_half], down.at[aligned(me * block, block)], local_sem.at[2]
        ),
        pltpu.make_async_copy(br_in, br.at[me], local_sem.at[3]),
        pltpu.make_async_copy(res_in, res.at[me_t], local_sem.at[4]),
        pltpu.make_async_copy(ow_in, ow.at[me_t], local_sem.at[5]),
    ]
    pl.semaphore_wait(barrier, n - 1 + 2 * (t - 1))

    @pl.when(can_up)
    def _():
        climb(KV, 1, 0, own=True).start()

    cross_kv(0).start()

    @pl.when(can_down)
    def _():
        sink(UP, 1, 0, own=True).start()

    cross_kv(1).start()
    cross(UP).start()
    cross(DOWN).start()

    def send_breaks(d, _):
        br_copy(d).start()
        return 0

    lax.fori_loop(1, n, send_breaks, 0)
    for c in locals_:
        c.start()
    spread_start(RES, res_at, res_in)
    spread_start(OW, ow_at, ow_in)

    key_row = lax.broadcasted_iota(jnp.int32, (tok, tok), 0)
    key_col = lax.broadcasted_iota(jnp.int32, (tok, tok), 1)
    lower[...] = jnp.where(key_row > key_col, 1.0, 0.0).astype(BF16)
    later_sum[...] = jnp.zeros_like(later_sum)
    totals[...] = jnp.zeros_like(totals)

    cross_kv(0, landed=True).wait_recv()

    @pl.when(can_up)
    def _():
        climb(KV, 1, 1).start()

    cross_kv(1, landed=True).wait_recv()
    cross(UP, landed=True).wait_recv()

    @pl.when(can_down)
    def _():
        sink(UP, 1, 1).start()

    def kv_event(hop, _):
        @pl.when(hop == layers - 1)
        def _():
            start_up(UP)

        kv_hop(hop)
        return 0

    lax.fori_loop(1, layers, kv_event, 0)
    spread_forward(RES, res_at)
    spread_forward(OW, ow_at)

    def kv_rest(hop, _):
        for piece in range(2):

            @pl.when(z - hop >= 0)
            def _():
                cross_kv_hop(hop, piece, landed=True).wait_recv()

        return 0

    lax.fori_loop(1, layers, kv_rest, 0)

    def wait_breaks(d, _):
        br_copy(d, landed=True).wait_recv()
        return 0

    lax.fori_loop(1, n, wait_breaks, 0)
    for c in locals_:
        c.wait()
    cross(DOWN, landed=True).wait_recv()

    scale = hd ** (-0.5)
    tile = 128

    def attend_block(j):
        b = me - j
        for h in range(heads):
            def rows(i, _):
                at = aligned(i * tile, tile)
                keys = kv[aligned(b * tok, tok), pl.ds(h * hd, hd)]
                vals = kv[aligned(b * tok, tok), pl.ds(width + h * hd, hd)]
                z = lax.dot_general(
                    q_ref[at, pl.ds(h * hd, hd)],
                    keys,
                    (((1,), (1,)), ((), ())),
                    preferred_element_type=F32,
                )
                z = z * scale + br[b, pl.ds(h, 1), :]
                soft = jnp.log(1.0 + jnp.exp(-jnp.abs(z)))
                log_break = jnp.minimum(z, 0.0) - soft
                r = lax.broadcasted_iota(jnp.int32, (tile, tok), 0) + i * tile + j * tok
                strict = lax.broadcasted_iota(jnp.int32, (tile, tok), 1) < r
                log_keep = jnp.where(strict, log_break - z, 0.0)
                high = log_keep.astype(BF16)
                low = (log_keep - high.astype(F32)).astype(BF16)
                tri = lower[...]
                later = jnp.dot(high, tri, preferred_element_type=F32) + jnp.dot(
                    low, tri, preferred_element_type=F32
                )
                before = later_sum[h, at, :]
                w = jnp.exp(log_break + later + before[:, 0:1])
                w = jnp.where(strict, w, 0.0).astype(BF16)
                totals[at, pl.ds(h * hd, hd)] += jnp.dot(w, vals, preferred_element_type=F32)
                later_sum[h, at, :] = before + jnp.sum(log_keep, axis=1, keepdims=True)
                return 0

            lax.fori_loop(0, tok // tile, rows, 0)

    def up_event(e):
        hop = 1 + e // 2
        for piece in range(2):

            @pl.when(lax.rem(jnp.int32(e), 2) == piece)
            def _():
                event(UP, hop, piece)

        @pl.when(jnp.int32(e) == 2 * layers - 4)
        def _():
            start_up(DOWN)
            start_down(DOWN)

    def attend_step(j, _):
        @pl.when(j <= me)
        def _():
            attend_block(j)

        @pl.when(j < 2 * layers - 5)
        def _():
            up_event(j)

        return 0

    lax.fori_loop(0, n, attend_step, 0)

    att_all[me_t] = totals[...].astype(BF16)
    spread_start(ATT, att_at)
    up_event(2 * layers - 5)
    spread_finish(OW, ow_at)
    spread_finish(RES, res_at)
    spread_forward(ATT, att_at)
    spread_finish(ATT, att_at)

    big = 256

    def mix_rows(i, _):
        at = aligned(i * big, big)
        for c in range(t):
            lanes = pl.ds(c * cols, cols)
            acc = ALPHA * res[c, at, :].astype(F32)
            mixed = jnp.zeros((big, cols), F32)
            for g in range(t):
                mixed = mixed + jnp.dot(
                    att_all[g, at, :], ow[g, :, lanes], preferred_element_type=F32
                ).astype(BF16).astype(F32)
            pre[at, lanes] = acc + mixed
        return 0

    lax.fori_loop(0, tok // big, mix_rows, 0)
    up_event(2 * layers - 4)

    small = 64

    def norm_rows(i, _):
        at = aligned(i * small, small)
        v = pre[at, :]
        center = jnp.sum(v, axis=1, keepdims=True) / feat
        v = v - center
        spread = jnp.sum(v * v, axis=1, keepdims=True) / feat
        first[y, at, :] = (v * lax.rsqrt(spread + EPSILON) * g1_ref[...] + b1_ref[...]).astype(BF16)
        return 0

    lax.fori_loop(0, tok // small, norm_rows, 0)

    def quarter(landed=False):
        dst = first.at[1 - y if landed else y, :, aligned(me_t * cols, cols)]
        return remote(dst, dst, quarter_send.at[0], quarter_recv.at[0], sp=partner)

    quarter().start()
    up_event(2 * layers - 3)
    event(DOWN, 1, 0)

    strip = 256

    def up_side(a):
        def up_cols(i, _):
            lanes = aligned(i * strip, strip)
            v = jnp.dot(first[a], up[:, lanes], preferred_element_type=F32)
            v = jnp.maximum(v, 0.0)
            activated[a, :, lanes] = (v * v).astype(BF16)
            return 0

        lax.fori_loop(0, part_hidden // strip, up_cols, 0)

    up_side(y)
    quarter(landed=True).wait_recv()
    spread_start(FIRST, far_at)
    event(DOWN, 1, 1)
    spread_forward(FIRST, far_at)
    spread_finish(FIRST, far_at)
    up_side(1 - y)

    def mix_copy(s, a):
        k = lax.rem(s, per)
        owner = s // per
        return owner, remote(
            part.at[s, a],
            mix.at[y * t + me_t, k],
            mix_send.at[s, a],
            mix_recv.at[y * t + me_t, k],
            sp=2 * z + a,
            tp=owner,
        )

    def down_block(s):
        def side(i, _):
            a = lax.rem(y + 1 + i, 2)
            v = lax.dot_general(
                activated[a],
                down[aligned(s * block, block), :],
                (((1,), (1,)), ((), ())),
                preferred_element_type=F32,
            ).astype(BF16)
            owner, copy = mix_copy(s, a)
            mine = jnp.logical_and(owner == me_t, a == y)

            @pl.when(mine)
            def _():
                mix[y * t + me_t, lax.rem(s, per)] = v

            @pl.when(jnp.logical_not(mine))
            def _():
                part[s, a] = v
                copy.start()

            return 0

        lax.fori_loop(0, 2, side, 0)

    down_block(me)
    down_block(partner)

    def down_step(hop, _):
        for piece in range(2):

            @pl.when(hop > 1)
            def _():
                event(DOWN, hop, piece)

            c = y if piece == 0 else 1 - y

            @pl.when(z - hop >= 0)
            def _():
                down_block(2 * (z - hop) + c)

            @pl.when(z + hop < layers)
            def _():
                down_block(2 * (z + hop) + c)

        return 0

    lax.fori_loop(1, layers, down_step, 0)

    def mix_wait(s, _):
        for a in range(2):
            owner, copy = mix_copy(s, a)

            @pl.when(jnp.logical_not(jnp.logical_and(owner == me_t, a == y)))
            def _():
                copy.wait_send()

        return 0

    def mix_landed(g, k):
        dst = mix.at[g, k]
        remote(dst, dst, mix_send.at[0, 0], mix_recv.at[g, k], sp=partner).wait_recv()

    for k in range(per):
        for d in range(1, t):
            mix_landed(y * t + lax.rem(me_t + t - d, t), k)
        for d in range(t):
            mix_landed((1 - y) * t + lax.rem(me_t + t - d, t), k)

    for i in range(tok // 128):
        at = pl.ds(i * 128, 128)
        v = ALPHA * first[y, at, aligned(me_t * cols, cols)].astype(F32)
        pieces = []
        for k in range(per):
            u = mix[0, k, at, :].astype(F32)
            for g in range(1, 2 * t):
                u = u + mix[g, k, at, :].astype(F32)
            pieces.append(u)
        v = v + (jnp.concatenate(pieces, axis=1) if per > 1 else pieces[0])
        pre[at, pl.ds(0, cols)] = v
        sums = jnp.sum(v, axis=1, keepdims=True)
        squares = jnp.sum(v * v, axis=1, keepdims=True)
        lane = lax.broadcasted_iota(jnp.int32, (128, 128), 1)
        both = jnp.where(lane == 0, sums, jnp.where(lane == 1, squares, 0.0))
        stat[me_t, :, at] = both.T[0:8, :]

    def stat_copy(d, landed=False):
        dst = stat.at[lax.rem(me_t + t - d, t) if landed else me_t]
        return remote(dst, dst, stat_send.at[d], stat_recv.at[d], tp=peer_t(d))

    for d in range(1, t):
        stat_copy(d).start()

    lax.fori_loop(0, n, mix_wait, 0)
    for item in (KV, UP, DOWN):
        drain_sends(item)
    cross_kv(0).wait_send()
    cross_kv(1).wait_send()
    cross(UP).wait_send()
    cross(DOWN).wait_send()
    quarter().wait_send()

    def br_done(d, _):
        br_copy(d).wait_send()
        return 0

    lax.fori_loop(1, n, br_done, 0)
    spread_drain(OW, ow_at)
    spread_drain(RES, res_at)
    spread_drain(ATT, att_at)
    spread_drain(FIRST, far_at)
    for d in range(1, t):
        stat_copy(d, landed=True).wait_recv()

    for i in range(tok // 128):
        at = pl.ds(i * 128, 128)
        v = stat[0, :, at]
        for g in range(1, t):
            v = v + stat[g, :, at]
        v = jnp.concatenate([v, jnp.zeros((120, 128), F32)], axis=0).T
        center = v[:, 0:1] / feat
        spread = v[:, 1:2] / feat - center * center
        u = (pre[at, pl.ds(0, cols)] - center) * lax.rsqrt(spread + EPSILON)
        out_ref[at, :] = (u * g2_ref[me_t] + b2_ref[me_t]).astype(BF16)
    for d in range(1, t):
        stat_copy(d).wait_send()


def solution(mesh):
    n, t = mesh.shape["sp"], mesh.shape["tp"]

    def body(
        queries,
        keys,
        values,
        breaks,
        residual_in,
        out_weight,
        first_gain,
        first_shift,
        up_weight,
        down_weight,
        second_gain,
        second_shift,
    ):
        tok, width = queries.shape
        heads = breaks.shape[1]
        feat = out_weight.shape[1]
        cols = residual_in.shape[1]
        hidden = up_weight.shape[1]
        block = up_weight.shape[0]
        per = n // t
        kv = jnp.concatenate([keys, values], axis=1)
        br = jnp.pad(breaks.astype(F32).T, ((0, 8 - heads), (0, 0)))
        any_ = pl.BlockSpec(memory_space=pl.ANY)
        vmem = pl.BlockSpec(memory_space=pltpu.VMEM)
        dma = pltpu.SemaphoreType.DMA
        ring = dma((3, n // 2 + 1, 2))
        return pl.pallas_call(
            functools.partial(layer_kernel, n, t, heads),
            out_shape=jax.ShapeDtypeStruct((tok, cols), BF16),
            in_specs=[vmem, any_, any_, any_, any_, vmem, vmem, any_, any_, vmem, vmem],
            out_specs=vmem,
            scratch_shapes=[
                pltpu.VMEM((n * tok, 2 * width), BF16),
                pltpu.VMEM((feat, hidden // 2), BF16),
                pltpu.VMEM((feat, hidden // 2), BF16),
                pltpu.VMEM((n, 8, tok), F32),
                pltpu.VMEM((t, width, feat), BF16),
                pltpu.VMEM((t, tok, cols), BF16),
                pltpu.VMEM((heads, tok, 128), F32),
                pltpu.VMEM((tok, width), F32),
                pltpu.VMEM((t, tok, width), BF16),
                pltpu.VMEM((tok, tok), BF16),
                pltpu.VMEM((tok, feat), F32),
                pltpu.VMEM((2, tok, feat), BF16),
                pltpu.VMEM((2, tok, hidden // 2), BF16),
                pltpu.VMEM((n, 2, tok, block), BF16),
                pltpu.VMEM((2 * t, per, tok, block), BF16),
                pltpu.VMEM((t, 8, tok), F32),
                ring,
                ring,
                ring,
                ring,
                dma((3,)),
                dma((3,)),
                dma((n // 2, 2)),
                dma((n // 2, 2)),
                dma((n,)),
                dma((n,)),
                dma((4, t)),
                dma((4, t)),
                dma((1,)),
                dma((1,)),
                dma((n, 2)),
                dma((2 * t, per)),
                dma((t,)),
                dma((t,)),
                dma((6,)),
            ],
            compiler_params=pltpu.CompilerParams(
                collective_id=0, has_side_effects=True, vmem_limit_bytes=62 * 1024 * 1024
            ),
        )(
            queries,
            kv,
            br,
            residual_in,
            out_weight,
            first_gain.reshape(1, feat),
            first_shift.reshape(1, feat),
            up_weight,
            down_weight,
            second_gain.reshape(t, 1, cols),
            second_shift.reshape(t, 1, cols),
        )

    return jax.shard_map(
        body,
        mesh=mesh,
        in_specs=(
            P("sp", "tp"),
            P("sp", "tp"),
            P("sp", "tp"),
            P("sp", "tp"),
            P("sp", "tp"),
            P("tp", None),
            P(),
            P(),
            P("sp", "tp"),
            P("sp", "tp"),
            P(),
            P(),
        ),
        out_specs=P("sp", "tp"),
        check_vma=False,
    )
```
